32 devices in a mesh: ra: 8 (over z, x), cb: 4 (over y, core).
Axes of the slice: x: 2, y: 2, z: 4, core: 2. Of those that a mesh axis runs over, the one named last changes fastest.
Arguments:
- inputs: bfloat16 [1536, 4096], P(None, 'ra'), may hold values from -12 to 12
- gate_weight: bfloat16 [2, 4096, 11264], P(None, 'ra', 'cb'), may hold values from -0.09375 to 0.09375
- up_weight: bfloat16 [2, 4096, 11264], P(None, 'ra', 'cb'), may hold values from -0.09375 to 0.09375
- down_weight: bfloat16 [2, 11264, 4096], P(None, 'cb', 'ra'), may hold values from -0.0546875 to 0.0546875
- norm_gain: float32 [2, 4096], P(None, 'ra'), may hold values from 0.05 to 8
- norm_shift: float32 [2, 4096], P(None, 'ra'), may hold values from -1.5 to 1.5
Outputs:
- outputs: bfloat16 [1536, 4096], P(None, 'ra')
The draws below stay inside these ranges and needn't reach their ends.
All inputs are finite; a program needn't handle non-finite values.
Results may differ from the reference program's by a relative error of at most 0.04.
Values may be sent and summed in bfloat16 or wider, within the bound.
A program may use at most 128 MiB of HBM per device.

```python
import jax
import jax.numpy as jnp
from jax import lax

D = 4096
FF = 11264
TOKENS = 1536
LAYERS = 2
N_RA = 8


def draw_inputs(key, part):
    key = jax.random.fold_in(key, 11)
    keys = jax.random.split(key, 3)
    groups = 32
    factor = jnp.exp(jax.random.uniform(keys[0], (1, groups), jnp.float32, jnp.log(0.3), jnp.log(3.0)))
    offset = jax.random.uniform(keys[1], (1, groups), jnp.float32, -1.0, 1.0)
    factor = jnp.repeat(factor, D // groups, axis=1)
    offset = jnp.repeat(offset, D // groups, axis=1)
    base = jax.random.normal(keys[2], (TOKENS, D), jnp.float32)
    return jnp.clip(base * factor + offset, -12.0, 12.0).astype(jnp.bfloat16)


def draw_norm_gain(key, part):
    key = jax.random.fold_in(key, 23)
    keys = jax.random.split(key, 2)
    groups = 32
    factor = jnp.exp(jax.random.uniform(keys[0], (LAYERS, groups), jnp.float32, jnp.log(0.35), jnp.log(3.0)))
    factor = jnp.repeat(factor, D // groups, axis=1)
    noise = jnp.clip(jax.random.normal(keys[1], (LAYERS, D), jnp.float32), -3.0, 3.0)
    return (factor * (1.0 + 0.18 * noise)).astype(jnp.float32)


def block_levels(stream_key, dims, pieces, low, high):
    level, own = 1.0, jax.random.fold_in(stream_key, 6)
    for axis_at, blocks in pieces:
        draws = jnp.exp(jax.random.uniform(jax.random.fold_in(own, axis_at), (blocks,), jnp.float32, low / len(pieces), high / len(pieces)))
        level = level * jnp.repeat(draws, dims[axis_at] // blocks).reshape([-1 if axis == axis_at else 1 for axis in range(len(dims))])
    return level


def scatter_about(key, shape, spread, most, pieces=(), dtype=jnp.bfloat16):
    loudness = block_levels(key, shape, pieces, -0.22, 0.18) if pieces else 1.0
    entries = jax.random.normal(key, shape, jnp.float32) * spread * loudness
    return jnp.minimum(jnp.maximum(entries, -most), most).astype(dtype)


def setup_inputs(seed: int = 0) -> dict:
    seeds = jax.random.split(jax.random.key(seed), 7)
    inputs = draw_inputs(jax.random.fold_in(seeds[6], 71), 0)
    gate_weight = scatter_about(seeds[1], (LAYERS, D, FF), D ** -0.5, 0.09375, ((1, 8), (2, 4)))
    up_weight = scatter_about(seeds[2], (LAYERS, D, FF), D ** -0.5, 0.09375, ((1, 8), (2, 4)))
    down_weight = scatter_about(seeds[3], (LAYERS, FF, D), FF ** -0.5, 0.0546875, ((1, 4), (2, 8)))
    norm_gain = draw_norm_gain(jax.random.fold_in(seeds[6], 71), 0)
    norm_shift = scatter_about(seeds[5], (LAYERS, D), 0.3, 1.5, ((1, 8),), jnp.float32)
    return {"inputs": inputs, "gate_weight": gate_weight, "up_weight": up_weight, "down_weight": down_weight, "norm_gain": norm_gain, "norm_shift": norm_shift}


RESIDUAL = 0.5
EPSILON = 1e-05

def block_products(stream, paired):
    width = D // N_RA
    total = jnp.zeros((stream.shape[0], paired.shape[1]), jnp.float32)
    for block_index in range(N_RA):
        start = block_index * width
        piece = jnp.dot(stream[:, start:start + width], paired[start:start + width], preferred_element_type=jnp.float32)
        rounded = lax.optimization_barrier(piece.astype(jnp.bfloat16))
        total = total + rounded.astype(jnp.float32)
    return total

def sublayer(stream, w_gate, w_up, w_down, gain_row, shift_row):
    columns = w_gate.shape[1]
    paired = jnp.concatenate((w_gate, w_up), axis=1)
    summed = block_products(stream, paired)
    hidden = (jax.nn.silu(summed[:, :columns]) * summed[:, columns:]).astype(jnp.bfloat16)
    branch = jnp.dot(hidden, w_down, preferred_element_type=jnp.float32)
    mixed_rows = RESIDUAL * stream.astype(jnp.float32) + branch
    mean_rows = lax.optimization_barrier(jnp.sum(mixed_rows, axis=1)) / D
    var_rows = lax.optimization_barrier(jnp.sum(mixed_rows * mixed_rows, axis=1)) / D - mean_rows * mean_rows
    normed = (mixed_rows - mean_rows[:, None]) * lax.rsqrt(var_rows + EPSILON)[:, None]
    return (normed * gain_row + shift_row).astype(jnp.bfloat16)

def reference(inputs, gate_weight, up_weight, down_weight, norm_gain, norm_shift):
    stream = inputs
    for layer_index in range(LAYERS):
        stream = sublayer(stream, gate_weight[layer_index], up_weight[layer_index], down_weight[layer_index], norm_gain[layer_index], norm_shift[layer_index])
    return stream
```

```python
import functools

import jax
import jax.numpy as jnp
from jax import lax
from jax.experimental import pallas as pl
from jax.experimental.pallas import tpu as pltpu
from jax.sharding import PartitionSpec as P

LAYERS = 2
RESIDUAL = 0.5
EPSILON = 1e-05
PAIR = 2
TOKEN_CHUNKS = 3
COLUMN_CHUNKS = 2
BF16 = jnp.bfloat16
F32 = jnp.float32


def dot(a, b):
    return jnp.dot(a, b, preferred_element_type=F32)


def axis_ring(total, stride, size):
    perm = []
    for i in range(total):
        at = (i // stride) % size
        perm.append((i, i + (((at + 1) % size) - at) * stride))
    return perm


def xor_perm(total, bit):
    return [(i, i ^ bit) for i in range(total)]


def swap(x, axis):
    return lax.ppermute(x, axis, xor_perm(lax.axis_size(axis), 1))


def part(x, at, size, dim=0):
    return lax.dynamic_slice_in_dim(x, at * size, size, dim)


def ring_reduce(block, axis, stride, size, me):
    perm = axis_ring(lax.axis_size(axis), stride, size)
    total = block(lax.rem(me + size - 1, size))
    for step in range(1, size):
        arrived = lax.ppermute(total.astype(BF16), axis, perm)
        total = arrived.astype(F32) + block(lax.rem(me + 2 * size - 1 - step, size))
    return total


def ring_gather(x, axis, stride, size, me):
    perm = axis_ring(lax.axis_size(axis), stride, size)
    rows = x.shape[0]
    whole = jnp.zeros((rows * size,) + x.shape[1:], x.dtype)
    whole = lax.dynamic_update_slice_in_dim(whole, x, me * rows, 0)
    for step in range(1, size):
        x = lax.ppermute(x, axis, perm)
        owner = lax.rem(me + size - step, size)
        whole = lax.dynamic_update_slice_in_dim(whole, x, owner * rows, 0)
    return whole


def swap_gather(x, axis, me):
    other = swap(x, axis)
    first = jnp.where(me == 0, x, other)
    second = jnp.where(me == 0, other, x)
    return jnp.concatenate((first, second), axis=0)


def sum_over_ra(stats):
    total = lax.axis_size("ra")
    if total & (total - 1):
        return lax.psum(stats, "ra")
    bit = 1
    while bit < total:
        stats = stats + lax.ppermute(stats, "ra", xor_perm(total, bit))
        bit *= 2
    return stats


def cuts_of(width):
    step = -(-width // COLUMN_CHUNKS)
    step = min(width, -(-step // 128) * 128)
    return [(s, min(step, width - s)) for s in range(0, width, step)]


def per_device(inputs, gate_weight, up_weight, down_weight, norm_gain, norm_shift):
    ra, cb = lax.axis_size("ra"), lax.axis_size("cb")
    r, c = lax.axis_index("ra"), lax.axis_index("cb")
    groups, rows_y = ra // PAIR, cb // 2
    q, g = lax.rem(r, PAIR), r // PAIR
    core, y = lax.rem(c, 2), c // 2
    tokens, width = inputs.shape
    full_width = width * ra
    columns = gate_weight.shape[2]
    half = columns // PAIR
    cuts = cuts_of(half)
    chunk = tokens // TOKEN_CHUNKS

    queue = [None]

    def queued_swap(away):
        if queue[0] is not None:
            away, queue[0] = lax.optimization_barrier((away, queue[0]))
        queue[0] = swap(away, "ra")
        return queue[0]

    def weights_of(layer):
        kept, sent = q * half, (1 - q) * half
        pairs, downs = [], []
        for start, size in cuts:
            own = jnp.concatenate(
                [lax.dynamic_slice(w, (layer, 0, kept + start), (1, width, size))[0] for w in (gate_weight, up_weight)], axis=1
            )
            away = jnp.concatenate(
                [lax.dynamic_slice(w, (layer, 0, sent + start), (1, width, size))[0] for w in (gate_weight, up_weight)], axis=1
            )
            pairs.append((own, queued_swap(away)))
        for start, size in cuts:
            own = lax.dynamic_slice(down_weight, (layer, kept + start, 0), (1, size, width))[0]
            away = lax.dynamic_slice(down_weight, (layer, sent + start, 0), (1, size, width))[0]
            downs.append((own, queued_swap(away)))
        return pairs, downs

    streams = []
    for k in range(TOKEN_CHUNKS):
        own = inputs[k * chunk:(k + 1) * chunk]
        over = swap(part(own, core, chunk // 2), "ra")
        streams.append((own, swap_gather(over, "cb", core)))

    gate_open = None
    for layer in range(LAYERS):
        pairs, downs = weights_of(layer)
        last = layer == LAYERS - 1
        after = []
        for own, other in streams:
            block_rows = chunk // groups
            outs_own, outs_other = 0.0, 0.0
            if gate_open is not None:
                own, other, _ = lax.optimization_barrier((own, other, gate_open))
            opened = []
            for (w_own, w_other), (d_own, d_other) in zip(pairs, downs):
                size = d_own.shape[0]

                def block(at):
                    return dot(part(own, at, block_rows), w_own) + dot(part(other, at, block_rows), w_other)

                total = ring_reduce(block, "ra", PAIR, groups, g)
                hidden = (jax.nn.silu(total[:, :size]) * total[:, size:]).astype(BF16)
                opened.append(hidden)
                hidden = ring_gather(hidden, "ra", PAIR, groups, g)
                outs_own = outs_own + dot(hidden, d_own)
                outs_other = outs_other + dot(hidden, d_other)
            gate_open = tuple(h[:1] for h in opened)
            out = jnp.concatenate((outs_own, outs_other), axis=1)
            out = part(out, core, chunk // 2) + swap(part(out, 1 - core, chunk // 2).astype(BF16), "cb").astype(F32)
            rows = chunk // cb
            out = ring_reduce(lambda at: part(out, at, rows), "cb", 2, rows_y, y)
            branch = out[:, :width] + swap(out[:, width:].astype(BF16), "ra").astype(F32)
            mine = lax.dynamic_slice_in_dim(own, core * (chunk // 2) + y * rows, rows, 0)
            mixed = RESIDUAL * mine.astype(F32) + branch
            stats = sum_over_ra(jnp.stack((jnp.sum(mixed, axis=1), jnp.sum(mixed * mixed, axis=1))))
            mean = stats[0] / full_width
            var = stats[1] / full_width - mean * mean
            normed = (mixed - mean[:, None]) * lax.rsqrt(var + EPSILON)[:, None]
            normed = (normed * norm_gain[layer] + norm_shift[layer]).astype(BF16)
            if not last:
                normed = jnp.concatenate((normed, swap(normed, "ra")), axis=1)
            whole = swap_gather(ring_gather(normed, "cb", 2, rows_y, y), "cb", core)
            after.append(whole if last else (whole[:, :width], whole[:, width:]))
        streams = after
    return jnp.concatenate(streams, axis=0)


UNIT = 128
TOKEN_PARTS = 3
HOP = 2
IN_FLIGHT = 4
MESH_ID = pl.DeviceIdType.MESH


def layer_kernel(
    groups, x_hbm, gate_hbm, up_hbm, down_hbm, gain, shift, out_hbm,
    wgu, wd, stream, sums, hid, acc, core_out, core_in, y_out, y_in, x_out, x_in, stat_out, stat_in,
    own_sem, wgu_send, wgu_recv, wd_send, wd_recv, sum_send, sum_recv, hid_send, hid_recv,
    core_send, core_recv, y_send, y_recv, x_send, x_recv, stat_send, stat_recv,
    xg_send, xg_recv, yg_send, yg_recv, cg_send, cg_recv, out_sem,
):
    n_ra = 2 * groups
    tokens, width = x_hbm.shape
    full_width = width * n_ra
    layers, nc = wgu.shape[0], wgu.shape[1]
    nt = acc.shape[0] // 2
    rows = acc.shape[1]
    half_rows, quarter = rows // 2, rows // 4
    used = nc * nt
    steps = used + layer_gap(groups, nc, nt)
    total = layers * steps
    units = nc * UNIT

    r, c = lax.axis_index("ra"), lax.axis_index("cb")
    q, g = lax.rem(r, 2), r // 2
    core, y = lax.rem(c, 2), c // 2
    x_peer = (r + 1 - 2 * q, c)
    y_peer = (r, (1 - y) * 2 + core)
    core_peer = (r, y * 2 + 1 - core)

    def place(h):
        p = (groups - 1 - g) if h == 0 else g
        ahead = (r - 2, c) if h == 0 else (r + 2, c)
        back = (r + 2, c) if h == 0 else (r - 2, c)
        return p, ahead, back

    def remote(src, dst, send, recv, to):
        return pltpu.make_async_remote_copy(src_ref=src, dst_ref=dst, send_sem=send, recv_sem=recv, device_id=to, device_id_type=MESH_ID)

    pairs = nc // 2
    odd = nc - 2 * pairs

    def order(n):
        layer = n // steps
        j = n - layer * steps
        first = layer == 0
        b, k = j // 3, lax.rem(j, 3)
        j3 = j - 3 * pairs - odd
        j4 = j3 - (nc - pairs)
        t_a = jnp.where(k == 2, 1, 0)
        c_a = jnp.where(k == 2, b, 2 * b + k)
        t_c = jnp.where(j4 < 0, 1, 2 + j4 // nc)
        c_c = jnp.where(j4 < 0, pairs + j3, lax.rem(jnp.maximum(j4, 0), nc))
        t_b = jnp.where(j3 < 0, 0, t_c)
        c_b = jnp.where(j3 < 0, nc - 1, c_c)
        t0 = jnp.where(j < 3 * pairs, t_a, t_b)
        c0 = jnp.where(j < 3 * pairs, c_a, c_b)
        t = jnp.where(first, t0, j // nc)
        cc = jnp.where(first, c0, lax.rem(j, nc))
        return layer, t, cc

    def valid(n):
        return (n >= 0) & (n < total) & (lax.rem(jnp.maximum(n, 0), steps) < used)

    def row_of(h, t):
        return pl.multiple_of(h * (nt * rows) + t * rows, rows)

    def rows_at(start, size):
        return pl.ds(pl.multiple_of(start, quarter), size)

    def gu_copy(layer, cc, which):
        src = gate_hbm if which == 0 else up_hbm
        cols = pl.ds(pl.multiple_of((1 - q) * units + cc * UNIT, UNIT), UNIT)
        return remote(
            src.at[layer, :, cols],
            wgu.at[layer, cc, pl.ds(width, width), pl.ds(which * UNIT, UNIT)],
            wgu_send.at[layer, cc, which], wgu_recv.at[layer, cc, which], x_peer,
        )

    def d_copy(layer, cc):
        src_rows = pl.ds(pl.multiple_of((1 - q) * units + cc * UNIT, UNIT), UNIT)
        return remote(
            down_hbm.at[layer, src_rows, :],
            wd.at[layer, cc, :, pl.ds(width, width)],
            wd_send.at[layer, cc], wd_recv.at[layer, cc], x_peer,
        )

    def send_gu(layer, cc):
        gu_copy(layer, cc, 0).start()
        gu_copy(layer, cc, 1).start()

    def own_gu(layer, cc, which):
        src = gate_hbm if which == 0 else up_hbm
        cols = pl.ds(pl.multiple_of(q * units + cc * UNIT, UNIT), UNIT)
        return pltpu.make_async_copy(
            src.at[layer, :, cols], wgu.at[layer, cc, pl.ds(0, width), pl.ds(which * UNIT, UNIT)], own_sem.at[0, layer, cc, which]
        )

    def own_d(layer, cc):
        src_rows = pl.ds(pl.multiple_of(q * units + cc * UNIT, UNIT), UNIT)
        return pltpu.make_async_copy(down_hbm.at[layer, src_rows, :], wd.at[layer, cc, :, pl.ds(0, width)], own_sem.at[1, layer, cc, 0])

    own_x = pltpu.make_async_copy(x_hbm, stream.at[:, pl.ds(0, width)], out_sem.at[0])

    other_cols = pl.ds(width, width)

    def first_x(h, t):
        mine = rows_at(row_of(h, t) + core * half_rows + y * quarter, quarter)
        return remote(x_hbm.at[mine, :], stream.at[mine, other_cols], xg_send.at[h, t], xg_recv.at[h, t], x_peer)

    def first_y(h, t):
        mine = rows_at(row_of(h, t) + core * half_rows + y * quarter, quarter)
        view = stream.at[mine, other_cols]
        return remote(view, view, yg_send.at[h, t], yg_recv.at[h, t], y_peer)

    def first_core(h, t):
        mine = rows_at(row_of(h, t) + core * half_rows, half_rows)
        view = stream.at[mine, other_cols]
        return remote(view, view, cg_send.at[h, t], cg_recv.at[h, t], core_peer)

    for t in range(nt):
        for h in range(2):
            first_x(h, t).start()
        if t == 0:
            own_x.start()
            send_gu(0, 0)
    for cc in range(1, min(IN_FLIGHT, nc)):
        send_gu(0, cc)

    def own_start(j, _):
        layer, cc = j // nc, lax.rem(j, nc)
        own_gu(layer, cc, 0).start()
        own_gu(layer, cc, 1).start()
        own_d(layer, cc).start()
        return 0

    def own_wait(j, _):
        layer, cc = j // nc, lax.rem(j, nc)
        own_gu(layer, cc, 0).wait()
        own_gu(layer, cc, 1).wait()
        own_d(layer, cc).wait()
        return 0

    lax.fori_loop(0, layers * nc, own_start, 0)
    for t in range(nt):
        for h in range(2):
            first_x(h, t).wait_recv()
            first_y(h, t).start()
    own_x.wait()
    for t in range(nt):
        for h in range(2):
            first_y(h, t).wait_recv()
            first_core(h, t).start()
    lax.fori_loop(0, layers * nc, own_wait, 0)
    for t in range(nt):
        for h in range(2):
            first_x(h, t).wait_send()
            first_y(h, t).wait_send()
            first_core(h, t).wait_send()

    def sum_copy(h, n):
        _, t, cc = order(n)
        _, ahead, _ = place(h)
        view = sums.at[h, t * nc + cc]
        return remote(view, view, sum_send.at[h, lax.rem(n, 4)], sum_recv.at[h, t * nc + cc], ahead)

    def hid_copy(h, n):
        _, t, cc = order(n)
        _, _, back = place(h)
        view = hid.at[h, t * nc + cc]
        return remote(view, view, hid_send.at[h, lax.rem(n, 4)], hid_recv.at[h, t * nc + cc], back)

    def stage_sum(h, n):
        p, _, _ = place(h)
        layer, t, cc = order(n)

        @pl.when((cc == 0) & (layer == 0))
        def _():
            first_core(h, t).wait_recv()

        @pl.when((cc == 0) & (layer > 0))
        def _():
            gather_core(h, t).wait_recv()

        slot = t * nc + cc
        own = jnp.dot(stream[pl.ds(row_of(h, t), rows), :], wgu[layer, cc], preferred_element_type=F32)

        @pl.when(p == 0)
        def _():
            sums[h, slot] = own.astype(BF16)

        @pl.when((p > 0) & (p < groups - 1))
        def _():
            sum_copy(h, n).wait_recv()
            sums[h, slot] = (sums[h, slot].astype(F32) + own).astype(BF16)

        @pl.when(p < groups - 1)
        def _():
            sum_copy(h, n).start()

        @pl.when(p == groups - 1)
        def _():
            sum_copy(h, n).wait_recv()
            whole = sums[h, slot].astype(F32) + own
            hid[h, slot] = (jax.nn.silu(whole[:, :UNIT]) * whole[:, UNIT:]).astype(BF16)

    def stage_hid(h, n):
        p, _, _ = place(h)

        @pl.when(p < groups - 1)
        def _():
            hid_copy(h, n).wait_recv()

        @pl.when(p > 0)
        def _():
            hid_copy(h, n).start()

    def stage_down(h, n):
        layer, t, cc = order(n)
        part_sum = jnp.dot(hid[h, t * nc + cc], wd[layer, cc], preferred_element_type=F32)
        m = h * nt + t

        @pl.when(cc == 0)
        def _():
            acc[m] = part_sum

        @pl.when(cc > 0)
        def _():
            acc[m] += part_sum

    def core_copy(h, t):
        m = h * nt + t
        return remote(core_out.at[m], core_in.at[m], core_send.at[h, t], core_recv.at[h, t], core_peer)

    def y_copy(h, t):
        m = h * nt + t
        return remote(y_out.at[m], y_in.at[m], y_send.at[h, t], y_recv.at[h, t], y_peer)

    def x_copy(h, t):
        m = h * nt + t
        return remote(x_out.at[m], x_in.at[m], x_send.at[h, t], x_recv.at[h, t], x_peer)

    def stat_copy(h, t, k):
        m = h * nt + t
        return remote(stat_out.at[m], stat_in.at[m, k], stat_send.at[h, t, k], stat_recv.at[h, t, k], (lax.rem(r + k, n_ra), c))

    def gather_x(h, t):
        mine = rows_at(row_of(h, t) + core * half_rows + y * quarter, quarter)
        return remote(stream.at[mine, pl.ds(0, width)], stream.at[mine, other_cols], xg_send.at[h, t], xg_recv.at[h, t], x_peer)

    def gather_y(h, t):
        mine = rows_at(row_of(h, t) + core * half_rows + y * quarter, quarter)
        return remote(stream.at[mine, :], stream.at[mine, :], yg_send.at[h, t], yg_recv.at[h, t], y_peer)

    def gather_core(h, t):
        mine = rows_at(row_of(h, t) + core * half_rows, half_rows)
        return remote(stream.at[mine, :], stream.at[mine, :], cg_send.at[h, t], cg_recv.at[h, t], core_peer)

    def out_copy(h, t):
        at = pl.ds(row_of(h, t), rows)
        return pltpu.make_async_copy(stream.at[at, pl.ds(0, width)], out_hbm.at[at, :], out_sem.at[1 + h * nt + t])

    kept_half = pl.multiple_of(core * half_rows, half_rows)
    sent_half = pl.multiple_of((1 - core) * half_rows, half_rows)
    kept = pl.multiple_of(core * half_rows + y * quarter, quarter)
    sent = pl.multiple_of(core * half_rows + (1 - y) * quarter, quarter)

    def end_core(h, layer, t):
        m = h * nt + t
        core_out[m] = acc[m, pl.ds(sent_half, half_rows), :].astype(BF16)
        core_copy(h, t).start()

    def end_y(h, layer, t):
        m = h * nt + t
        core_copy(h, t).wait()
        acc[m, pl.ds(kept_half, half_rows), :] += core_in[m].astype(F32)
        y_out[m] = acc[m, pl.ds(sent, quarter), :].astype(BF16)
        y_copy(h, t).start()

    def end_x(h, layer, t):
        m = h * nt + t
        y_copy(h, t).wait()
        acc[m, pl.ds(kept, quarter), :] += y_in[m].astype(F32)
        x_out[m] = acc[m, pl.ds(kept, quarter), pl.ds(width, width)].astype(BF16)
        x_copy(h, t).start()

    def lane_fold(v):
        total_v = v[:, :UNIT]
        for at in range(UNIT, width, UNIT):
            total_v = total_v + v[:, at:at + UNIT]
        return total_v

    def across(a, b):
        return lax.dot_general(a, b, (((1,), (1,)), ((), ())), preferred_element_type=F32, precision=lax.Precision.HIGHEST)

    def end_stats(h, layer, t):
        m = h * nt + t
        x_copy(h, t).wait()
        branch = acc[m, pl.ds(kept, quarter), pl.ds(0, width)] + x_in[m].astype(F32)
        mine = stream[rows_at(row_of(h, t) + kept, quarter), pl.ds(0, width)]
        mixed = RESIDUAL * mine.astype(F32) + branch
        acc[m, pl.ds(kept, quarter), pl.ds(0, width)] = mixed
        ones = jnp.ones((8, UNIT), F32)
        plain = across(ones, lane_fold(mixed))
        squared = across(ones, lane_fold(mixed * mixed))
        at = lax.broadcasted_iota(jnp.int32, plain.shape, 0)
        stat_out[m] = jnp.where(at < 4, plain, squared)
        for k in range(1, n_ra):
            stat_copy(h, t, k).start()

    def end_norm(h, layer, t):
        m = h * nt + t
        whole = stat_out[m]
        for k in range(1, n_ra):
            stat_copy(h, t, k).wait()
            whole = whole + stat_in[m, k]
        eye = (lax.broadcasted_iota(jnp.int32, (quarter, quarter), 0) == lax.broadcasted_iota(jnp.int32, (quarter, quarter), 1)).astype(F32)
        turned = across(eye, whole)
        mean = turned[:, 0:1] / full_width
        var = turned[:, 4:5] / full_width - mean * mean
        mixed = acc[m, pl.ds(kept, quarter), pl.ds(0, width)]
        normed = (mixed - mean) * lax.rsqrt(var + EPSILON)
        normed = normed * gain[pl.ds(layer, 1), :] + shift[pl.ds(layer, 1), :]
        stream[rows_at(row_of(h, t) + kept, quarter), pl.ds(0, width)] = normed.astype(BF16)

        @pl.when(layer < layers - 1)
        def _():
            gather_x(h, t).start()

    def end_gather_y(h, layer, t):
        @pl.when(layer < layers - 1)
        def _():
            gather_x(h, t).wait()

        gather_y(h, t).start()

    def end_gather_core(h, layer, t):
        gather_y(h, t).wait()
        gather_core(h, t).start()

    def end_sent(h, layer, t):
        gather_core(h, t).wait_send()

        @pl.when(layer == layers - 1)
        def _():
            gather_core(h, t).wait_recv()
            out_copy(h, t).start()

    longest = HOP * 2 * (groups - 1)

    def lag_hid(h):
        return longest - HOP * place(h)[0]

    stages = (
        (lambda h: lag_hid(h), end_core),
        (lambda h: lag_hid(h) + ENDS[0], end_y),
        (lambda h: lag_hid(h) + ENDS[1], end_x),
        (lambda h: lag_hid(h) + ENDS[2], end_stats),
        (lambda h: longest + ENDS[3], end_norm),
        (lambda h: longest + ENDS[4], end_gather_y),
        (lambda h: longest + ENDS[5], end_gather_core),
        (lambda h: longest + ENDS[6], end_sent),
    )

    p0, p1 = place(0)[0], place(1)[0]
    p_low, p_high = jnp.minimum(p0, p1), jnp.maximum(p0, p1)

    def weight_message(w):
        layer = w // (2 * nc)
        k = w - layer * 2 * nc
        lead = jnp.where(layer == 0, IN_FLIGHT, 1)
        mid = k - lead
        in_mid = (mid >= 0) & (mid < 2 * (nc - lead))
        is_gu = (k < lead) | (in_mid & (lax.rem(jnp.maximum(mid, 0), 2) == 1))
        gu_at = jnp.where(k < lead, k, lead + mid // 2)
        d_at = jnp.where(in_mid, mid // 2, k - nc)
        return layer, is_gu, gu_at, d_at

    n_messages = 2 * nc * layers

    def issue_weights(w):
        layer, is_gu, gu_at, d_at = weight_message(w)

        @pl.when(is_gu)
        def _():
            send_gu(layer, gu_at)

        @pl.when(jnp.logical_not(is_gu))
        def _():
            d_copy(layer, d_at).start()

    def sent_weights(w):
        layer, is_gu, gu_at, d_at = weight_message(w)

        @pl.when(is_gu)
        def _():
            gu_copy(layer, gu_at, 0).wait_send()
            gu_copy(layer, gu_at, 1).wait_send()

        @pl.when(jnp.logical_not(is_gu))
        def _():
            d_copy(layer, d_at).wait_send()

    fast = 2 * nc - IN_FLIGHT

    def body(i, _):
        j = i - fast
        slow = (j >= 0) & (lax.rem(jnp.maximum(j, 0), 5) < 4)
        w = jnp.where(j < 0, IN_FLIGHT + i, 2 * nc + (j // 5) * 4 + lax.rem(jnp.maximum(j, 0), 5))

        @pl.when(((j < 0) | slow) & (w < n_messages))
        def _():
            sent_weights(w - IN_FLIGHT)
            issue_weights(w)

        n_w = i - HOP * p_low
        layer_w, t_w, c_w = order(n_w)

        @pl.when(valid(n_w) & (t_w == 0))
        def _():
            gu_copy(layer_w, c_w, 0).wait_recv()
            gu_copy(layer_w, c_w, 1).wait_recv()

        n_d = i - longest + HOP * p_high
        layer_d, t_d, c_d = order(n_d)

        @pl.when(valid(n_d) & (t_d == 0))
        def _():
            d_copy(layer_d, c_d).wait_recv()

        for h in range(2):
            p, _, _ = place(h)
            n_s = i - HOP * p
            n_h = i - lag_hid(h)

            @pl.when(valid(n_s - 2) & (p < groups - 1))
            def _(h=h, n=n_s - 2):
                sum_copy(h, n).wait_send()

            @pl.when(valid(n_h - 2) & (p > 0))
            def _(h=h, n=n_h - 2):
                hid_copy(h, n).wait_send()

            @pl.when(valid(n_h) & (p < groups - 1))
            def _(h=h, n=n_h):
                stage_hid(h, n)

        for h in range(2):
            p, _, _ = place(h)
            n_s = i - HOP * p

            @pl.when(valid(n_s))
            def _(h=h, n=n_s):
                stage_sum(h, n)

            @pl.when(valid(n_s) & (p == groups - 1))
            def _(h=h, n=n_s):
                stage_hid(h, n)

        for h in range(2):
            n_h = i - lag_hid(h)

            @pl.when(valid(n_h))
            def _(h=h, n=n_h):
                stage_down(h, n)

        for lag, stage in stages:
            for h in range(2):
                n_e = i - lag(h)
                layer_e, t_e, c_e = order(n_e)

                @pl.when(valid(n_e) & (c_e == nc - 1))
                def _(h=h, stage=stage, layer_e=layer_e, t_e=t_e):
                    stage(h, layer_e, t_e)

        return 0

    lax.fori_loop(0, total + longest + ENDS[6], body, 0)
    for w in range(n_messages - IN_FLIGHT, n_messages):
        sent_weights(jnp.int32(w))
    for t in range(nt):
        for h in range(2):
            out_copy(h, t).wait()


ENDS = (1, 3, 5, 7, 9, 11, 12)


def layer_gap(groups, nc, nt):
    after = HOP * 2 * (groups - 1) + ENDS[5] + 1
    pairs = nc // 2
    ends = [2 * pairs + pairs - 2 if nc == 2 * pairs else 3 * pairs]
    ends += [3 * pairs + (nc - 2 * pairs) + (nc - pairs) - 1]
    ends += [t * nc + nc - 1 for t in range(2, nt)]
    return max([0] + [ends[t] + after - (nc * nt + t * nc) for t in range(nt)])


def fits(ra, cb, tokens, width, columns):
    units = columns // PAIR
    return (
        ra % PAIR == 0 and ra >= 2 * PAIR and cb == 4 and units % UNIT == 0 and units // UNIT > IN_FLIGHT
        and width % UNIT == 0 and tokens % (2 * TOKEN_PARTS * 4 * 16) == 0
    )


def per_device_kernel(inputs, gate_weight, up_weight, down_weight, norm_gain, norm_shift):
    ra = lax.axis_size("ra")
    tokens, width = inputs.shape
    layers, _, columns = gate_weight.shape
    groups, units = ra // PAIR, columns // PAIR
    nc, nt = units // UNIT, TOKEN_PARTS
    rows = tokens // (2 * nt)
    slots, chunks = nc * nt, 2 * nt
    dma = pltpu.SemaphoreType.DMA
    scratch = [
        pltpu.VMEM((layers, nc, 2 * width, 2 * UNIT), BF16),
        pltpu.VMEM((layers, nc, UNIT, 2 * width), BF16),
        pltpu.VMEM((tokens, 2 * width), BF16),
        pltpu.VMEM((2, slots, rows, 2 * UNIT), BF16),
        pltpu.VMEM((2, slots, rows, UNIT), BF16),
        pltpu.VMEM((chunks, rows, 2 * width), F32),
        pltpu.VMEM((chunks, rows // 2, 2 * width), BF16),
        pltpu.VMEM((chunks, rows // 2, 2 * width), BF16),
        pltpu.VMEM((chunks, rows // 4, 2 * width), BF16),
        pltpu.VMEM((chunks, rows // 4, 2 * width), BF16),
        pltpu.VMEM((chunks, rows // 4, width), BF16),
        pltpu.VMEM((chunks, rows // 4, width), BF16),
        pltpu.VMEM((chunks, 8, rows // 4), F32),
        pltpu.VMEM((chunks, ra, 8, rows // 4), F32),
        dma((2, layers, nc, 2)),
        dma((layers, nc, 2)), dma((layers, nc, 2)), dma((layers, nc)), dma((layers, nc)),
        dma((2, 4)), dma((2, slots)), dma((2, 4)), dma((2, slots)),
        dma((2, nt)), dma((2, nt)), dma((2, nt)), dma((2, nt)), dma((2, nt)), dma((2, nt)),
        dma((2, nt, ra)), dma((2, nt, ra)),
        dma((2, nt)), dma((2, nt)), dma((2, nt)), dma((2, nt)), dma((2, nt)), dma((2, nt)),
        dma((1 + chunks,)),
    ]
    anywhere, near = pl.BlockSpec(memory_space=pl.ANY), pl.BlockSpec(memory_space=pltpu.VMEM)
    return pl.pallas_call(
        functools.partial(layer_kernel, groups),
        out_shape=jax.ShapeDtypeStruct((tokens, width), BF16),
        in_specs=[anywhere] * 4 + [near] * 2,
        out_specs=anywhere,
        scratch_shapes=scratch,
        compiler_params=pltpu.CompilerParams(has_side_effects=True, vmem_limit_bytes=62 * 2**20),
    )(inputs, gate_weight, up_weight, down_weight, norm_gain, norm_shift)


def per_device_any(inputs, gate_weight, up_weight, down_weight, norm_gain, norm_shift):
    ra, cb = lax.axis_size("ra"), lax.axis_size("cb")
    run = per_device_kernel if fits(ra, cb, *inputs.shape, gate_weight.shape[2]) else per_device
    return run(inputs, gate_weight, up_weight, down_weight, norm_gain, norm_shift)


def solution(mesh):
    return jax.shard_map(
        per_device_any,
        mesh=mesh,
        in_specs=(
            P(None, "ra"),
            P(None, "ra", "cb"),
            P(None, "ra", "cb"),
            P(None, "cb", "ra"),
            P(None, "ra"),
            P(None, "ra"),
        ),
        out_specs=P(None, "ra"),
        check_vma=False,
    )
```

```python
import functools

import jax
import jax.numpy as jnp
from jax import lax
from jax.experimental import pallas as pl
from jax.experimental.pallas import tpu as pltpu
from jax.sharding import PartitionSpec as P

LAYERS = 2
RESIDUAL = 0.5
EPSILON = 1e-05
PAIR = 2
TOKEN_CHUNKS = 3
COLUMN_CHUNKS = 2
BF16 = jnp.bfloat16
F32 = jnp.float32


def dot(a, b):
    return jnp.dot(a, b, preferred_element_type=F32)


def axis_ring(total, stride, size):
    perm = []
    for i in range(total):
        at = (i // stride) % size
        perm.append((i, i + (((at + 1) % size) - at) * stride))
    return perm


def xor_perm(total, bit):
    return [(i, i ^ bit) for i in range(total)]


def swap(x, axis):
    return lax.ppermute(x, axis, xor_perm(lax.axis_size(axis), 1))


def part(x, at, size, dim=0):
    return lax.dynamic_slice_in_dim(x, at * size, size, dim)


def ring_reduce(block, axis, stride, size, me):
    perm = axis_ring(lax.axis_size(axis), stride, size)
    total = block(lax.rem(me + size - 1, size))
    for step in range(1, size):
        arrived = lax.ppermute(total.astype(BF16), axis, perm)
        total = arrived.astype(F32) + block(lax.rem(me + 2 * size - 1 - step, size))
    return total


def ring_gather(x, axis, stride, size, me):
    perm = axis_ring(lax.axis_size(axis), stride, size)
    rows = x.shape[0]
    whole = jnp.zeros((rows * size,) + x.shape[1:], x.dtype)
    whole = lax.dynamic_update_slice_in_dim(whole, x, me * rows, 0)
    for step in range(1, size):
        x = lax.ppermute(x, axis, perm)
        owner = lax.rem(me + size - step, size)
        whole = lax.dynamic_update_slice_in_dim(whole, x, owner * rows, 0)
    return whole


def swap_gather(x, axis, me):
    other = swap(x, axis)
    first = jnp.where(me == 0, x, other)
    second = jnp.where(me == 0, other, x)
    return jnp.concatenate((first, second), axis=0)


def sum_over_ra(stats):
    total = lax.axis_size("ra")
    if total & (total - 1):
        return lax.psum(stats, "ra")
    bit = 1
    while bit < total:
        stats = stats + lax.ppermute(stats, "ra", xor_perm(total, bit))
        bit *= 2
    return stats


def cuts_of(width):
    step = -(-width // COLUMN_CHUNKS)
    step = min(width, -(-step // 128) * 128)
    return [(s, min(step, width - s)) for s in range(0, width, step)]


def per_device(inputs, gate_weight, up_weight, down_weight, norm_gain, norm_shift):
    ra, cb = lax.axis_size("ra"), lax.axis_size("cb")
    r, c = lax.axis_index("ra"), lax.axis_index("cb")
    groups, rows_y = ra // PAIR, cb // 2
    q, g = lax.rem(r, PAIR), r // PAIR
    core, y = lax.rem(c, 2), c // 2
    tokens, width = inputs.shape
    full_width = width * ra
    columns = gate_weight.shape[2]
    half = columns // PAIR
    cuts = cuts_of(half)
    chunk = tokens // TOKEN_CHUNKS

    queue = [None]

    def queued_swap(away):
        if queue[0] is not None:
            away, queue[0] = lax.optimization_barrier((away, queue[0]))
        queue[0] = swap(away, "ra")
        return queue[0]

    def weights_of(layer):
        kept, sent = q * half, (1 - q) * half
        pairs, downs = [], []
        for start, size in cuts:
            own = jnp.concatenate(
                [lax.dynamic_slice(w, (layer, 0, kept + start), (1, width, size))[0] for w in (gate_weight, up_weight)], axis=1
            )
            away = jnp.concatenate(
                [lax.dynamic_slice(w, (layer, 0, sent + start), (1, width, size))[0] for w in (gate_weight, up_weight)], axis=1
            )
            pairs.append((own, queued_swap(away)))
        for start, size in cuts:
            own = lax.dynamic_slice(down_weight, (layer, kept + start, 0), (1, size, width))[0]
            away = lax.dynamic_slice(down_weight, (layer, sent + start, 0), (1, size, width))[0]
            downs.append((own, queued_swap(away)))
        return pairs, downs

    streams = []
    for k in range(TOKEN_CHUNKS):
        own = inputs[k * chunk:(k + 1) * chunk]
        over = swap(part(own, core, chunk // 2), "ra")
        streams.append((own, swap_gather(over, "cb", core)))

    gate_open = None
    for layer in range(LAYERS):
        pairs, downs = weights_of(layer)
        last = layer == LAYERS - 1
        after = []
        for own, other in streams:
            block_rows = chunk // groups
            outs_own, outs_other = 0.0, 0.0
            if gate_open is not None:
                own, other, _ = lax.optimization_barrier((own, other, gate_open))
            opened = []
            for (w_own, w_other), (d_own, d_other) in zip(pairs, downs):
                size = d_own.shape[0]

                def block(at):
                    return dot(part(own, at, block_rows), w_own) + dot(part(other, at, block_rows), w_other)

                total = ring_reduce(block, "ra", PAIR, groups, g)
                hidden = (jax.nn.silu(total[:, :size]) * total[:, size:]).astype(BF16)
                opened.append(hidden)
                hidden = ring_gather(hidden, "ra", PAIR, groups, g)
                outs_own = outs_own + dot(hidden, d_own)
                outs_other = outs_other + dot(hidden, d_other)
            gate_open = tuple(h[:1] for h in opened)
            out = jnp.concatenate((outs_own, outs_other), axis=1)
            out = part(out, core, chunk // 2) + swap(part(out, 1 - core, chunk // 2).astype(BF16), "cb").astype(F32)
            rows = chunk // cb
            out = ring_reduce(lambda at: part(out, at, rows), "cb", 2, rows_y, y)
            branch = out[:, :width] + swap(out[:, width:].astype(BF16), "ra").astype(F32)
            mine = lax.dynamic_slice_in_dim(own, core * (chunk // 2) + y * rows, rows, 0)
            mixed = RESIDUAL * mine.astype(F32) + branch
            stats = sum_over_ra(jnp.stack((jnp.sum(mixed, axis=1), jnp.sum(mixed * mixed, axis=1))))
            mean = stats[0] / full_width
            var = stats[1] / full_width - mean * mean
            normed = (mixed - mean[:, None]) * lax.rsqrt(var + EPSILON)[:, None]
            normed = (normed * norm_gain[layer] + norm_shift[layer]).astype(BF16)
            if not last:
                normed = jnp.concatenate((normed, swap(normed, "ra")), axis=1)
            whole = swap_gather(ring_gather(normed, "cb", 2, rows_y, y), "cb", core)
            after.append(whole if last else (whole[:, :width], whole[:, width:]))
        streams = after
    return jnp.concatenate(streams, axis=0)


UNIT = 128
TOKEN_PARTS = 3
HOP = 3
BACK = 3
SENT = 4
LEAD = 2
AHEAD = 6
IN_FLIGHT = 4
EARLY_OF = 4
LATE_OF = 7
LATE = (6, 10, 14)
MESH_ID = pl.DeviceIdType.MESH


def layer_kernel(
    groups, x_hbm, gate_hbm, up_hbm, down_hbm, gain, shift, out_hbm,
    wgu, wd, stream, sums, hid, acc, core_out, core_in, plane_out, plane_in, stat_out, stat_in,
    own_sem, wgu_send, wgu_recv, wd_send, wd_recv, sum_send, sum_recv, hid_send, hid_recv,
    core_send, core_recv, plane_send, plane_recv, stat_send, stat_recv,
    xg_send, xg_recv, yg_send, yg_recv, dg_send, dg_recv, cg_send, cg_recv, out_sem,
):
    n_ra = 2 * groups
    tokens, width = x_hbm.shape
    full_width = width * n_ra
    layers, nc = wgu.shape[0], wgu.shape[1]
    nt = acc.shape[0] // 2
    rows = acc.shape[1]
    half_rows, quarter = rows // 2, rows // 4
    used = nc * nt
    steps = 2 * used + layer_gap(groups, nc, nt)
    units = nc * UNIT

    r, c = lax.axis_index("ra"), lax.axis_index("cb")
    q, g = lax.rem(r, 2), r // 2
    core, y = lax.rem(c, 2), c // 2
    x_peer = (r + 1 - 2 * q, c)
    y_peer = (r, (1 - y) * 2 + core)
    core_peer = (r, y * 2 + 1 - core)
    far_peer = (x_peer[0], y_peer[1])

    def place(h):
        p = (groups - 1 - g) if h == 0 else g
        ahead = (r - 2, c) if h == 0 else (r + 2, c)
        back = (r + 2, c) if h == 0 else (r - 2, c)
        return p, ahead, back

    def remote(src, dst, send, recv, to):
        return pltpu.make_async_remote_copy(src_ref=src, dst_ref=dst, send_sem=send, recv_sem=recv, device_id=to, device_id_type=MESH_ID)

    def order(j):
        both = j < 2 * nc
        return jnp.where(both, lax.rem(j, 2), j // nc), jnp.where(both, j // 2, lax.rem(j, nc))

    def at_step(s, lag):
        n = s - lag
        layer = jnp.maximum(n, 0) // steps
        j2 = n - layer * steps
        return (n >= 0) & (layer < layers) & (j2 < 2 * used) & (lax.rem(jnp.maximum(j2, 0), 2) == 0), layer, j2 // 2

    def row_of(h, t):
        return pl.multiple_of(h * (nt * rows) + t * rows, rows)

    def rows_at(start, size):
        return pl.ds(pl.multiple_of(start, quarter), size)

    def gu_copy(layer, cc, which):
        src = gate_hbm if which == 0 else up_hbm
        cols = pl.ds(pl.multiple_of((1 - q) * units + cc * UNIT, UNIT), UNIT)
        return remote(
            src.at[layer, :, cols],
            wgu.at[layer, cc, pl.ds(width, width), pl.ds(which * UNIT, UNIT)],
            wgu_send.at[layer, cc, which], wgu_recv.at[layer, cc, which], x_peer,
        )

    def d_copy(layer, cc):
        src_rows = pl.ds(pl.multiple_of((1 - q) * units + cc * UNIT, UNIT), UNIT)
        return remote(
            down_hbm.at[layer, src_rows, :],
            wd.at[layer, cc, :, pl.ds(width, width)],
            wd_send.at[layer, cc], wd_recv.at[layer, cc], x_peer,
        )

    per_layer = 3 * nc
    n_messages = layers * per_layer

    def message(w, act):
        layer = w // per_layer
        k = w - layer * per_layer
        k2 = k - 2 * LEAD
        k3 = k2 - 3 * (nc - LEAD)
        m = jnp.maximum(k2, 0) // 3
        turn = jnp.maximum(k2, 0) - 3 * m
        early = k2 < 0
        is_down = jnp.logical_not(early) & ((k3 >= 0) | (turn == 0))
        which = jnp.where(early, lax.rem(k, 2), turn - 1)
        gu_at = jnp.where(early, k // 2, LEAD + m)
        d_at = jnp.where(k3 >= 0, nc - LEAD + k3, m)

        @pl.when(is_down)
        def _():
            act(d_copy(layer, d_at))

        for part_at in range(2):
            @pl.when(jnp.logical_not(is_down) & (which == part_at))
            def _(part_at=part_at):
                act(gu_copy(layer, gu_at, part_at))

    def issue(w):
        message(w, lambda copy: copy.start())

    def issued(w):
        message(w, lambda copy: copy.wait_send())

    def own_gu(layer, cc, which):
        src = gate_hbm if which == 0 else up_hbm
        cols = pl.ds(pl.multiple_of(q * units + cc * UNIT, UNIT), UNIT)
        return pltpu.make_async_copy(
            src.at[layer, :, cols], wgu.at[layer, cc, pl.ds(0, width), pl.ds(which * UNIT, UNIT)], own_sem.at[0, layer, cc, which]
        )

    def own_d(layer, cc):
        src_rows = pl.ds(pl.multiple_of(q * units + cc * UNIT, UNIT), UNIT)
        return pltpu.make_async_copy(down_hbm.at[layer, src_rows, :], wd.at[layer, cc, :, pl.ds(0, width)], own_sem.at[1, layer, cc, 0])

    own_x = pltpu.make_async_copy(x_hbm, stream.at[:, pl.ds(0, width)], out_sem.at[0])

    other_cols = pl.ds(width, width)

    def first_x(h, t):
        mine = rows_at(row_of(h, t) + core * half_rows + y * quarter, quarter)
        return remote(x_hbm.at[mine, :], stream.at[mine, other_cols], xg_send.at[h, t], xg_recv.at[h, t], x_peer)

    def first_y(h, t):
        mine = rows_at(row_of(h, t) + core * half_rows + y * quarter, quarter)
        view = stream.at[mine, other_cols]
        return remote(view, view, yg_send.at[h, t], yg_recv.at[h, t], y_peer)

    def first_core(h, t):
        mine = rows_at(row_of(h, t) + core * half_rows, half_rows)
        view = stream.at[mine, other_cols]
        return remote(view, view, cg_send.at[h, t], cg_recv.at[h, t], core_peer)

    soon = min(2, nt)
    for t in range(soon):
        for h in range(2):
            first_x(h, t).start()
    own_x.start()
    for w in range(AHEAD):
        issue(jnp.int32(w))
        if w == 1:
            for t in range(soon, nt):
                for h in range(2):
                    first_x(h, t).start()

    def pass_y(chunks):
        for t in chunks:
            for h in range(2):
                first_x(h, t).wait_recv()
                first_y(h, t).start()

    def pass_core(chunks):
        for t in chunks:
            for h in range(2):
                first_y(h, t).wait_recv()
                first_core(h, t).start()

    def passed(chunks):
        for t in chunks:
            for h in range(2):
                first_x(h, t).wait_send()
                first_y(h, t).wait_send()
                first_core(h, t).wait_send()

    def own_start(j, _):
        layer, cc = j // nc, lax.rem(j, nc)
        own_gu(layer, cc, 0).start()
        own_gu(layer, cc, 1).start()
        own_d(layer, cc).start()
        return 0

    def own_wait(j, _):
        layer, cc = j // nc, lax.rem(j, nc)
        own_gu(layer, cc, 0).wait()
        own_gu(layer, cc, 1).wait()
        own_d(layer, cc).wait()
        return 0

    lax.fori_loop(0, layers * nc, own_start, 0)
    pass_y(range(soon))
    own_x.wait()
    pass_core(range(soon))
    lax.fori_loop(0, layers * nc, own_wait, 0)
    passed(range(soon))
    for w in range(AHEAD - IN_FLIGHT):
        issued(jnp.int32(w))

    def sum_copy(h, layer, j):
        t, cc = order(j)
        _, ahead, _ = place(h)
        view = sums.at[h, t * nc + cc]
        return remote(view, view, sum_send.at[h, lax.rem(layer * used + j, 4)], sum_recv.at[h, t * nc + cc], ahead)

    def hid_copy(h, layer, j):
        t, cc = order(j)
        _, _, back = place(h)
        view = hid.at[h, t * nc + cc]
        return remote(view, view, hid_send.at[h, lax.rem(layer * used + j, 4)], hid_recv.at[h, t * nc + cc], back)

    def stage_sum(h, layer, j):
        p, _, _ = place(h)
        t, cc = order(j)

        @pl.when((cc == 0) & (layer == 0))
        def _():
            first_core(h, t).wait_recv()

        @pl.when((cc == 0) & (layer > 0))
        def _():
            gather_core(h, t, False).wait_recv()

        slot = t * nc + cc
        own = jnp.dot(stream[pl.ds(row_of(h, t), rows), :], wgu[layer, cc], preferred_element_type=F32)

        @pl.when(p == 0)
        def _():
            sums[h, slot] = own.astype(BF16)

        @pl.when((p > 0) & (p < groups - 1))
        def _():
            sum_copy(h, layer, j).wait_recv()
            sums[h, slot] = (sums[h, slot].astype(F32) + own).astype(BF16)

        @pl.when(p < groups - 1)
        def _():
            sum_copy(h, layer, j).start()

        @pl.when(p == groups - 1)
        def _():
            sum_copy(h, layer, j).wait_recv()
            whole = sums[h, slot].astype(F32) + own
            hid[h, slot] = (jax.nn.silu(whole[:, :UNIT]) * whole[:, UNIT:]).astype(BF16)

    def stage_hid(h, layer, j):
        p, _, _ = place(h)

        @pl.when(p < groups - 1)
        def _():
            hid_copy(h, layer, j).wait_recv()

        @pl.when(p > 0)
        def _():
            hid_copy(h, layer, j).start()

    def stage_down(h, layer, j):
        t, cc = order(j)
        part_sum = jnp.dot(hid[h, t * nc + cc], wd[layer, cc], preferred_element_type=F32)
        m = h * nt + t

        @pl.when(cc == 0)
        def _():
            acc[m] = part_sum

        @pl.when(cc > 0)
        def _():
            acc[m] += part_sum

    def core_copy(h, t):
        m = h * nt + t
        return remote(core_out.at[m], core_in.at[m], core_send.at[h, t], core_recv.at[h, t], core_peer)

    def plane_copy(h, t, k):
        m = h * nt + t
        return remote(
            plane_out.at[m, k], plane_in.at[m, k], plane_send.at[h, t, k], plane_recv.at[h, t, k], (x_peer, y_peer, far_peer)[k]
        )

    def stat_copy(h, t, k):
        m = h * nt + t
        return remote(stat_out.at[m], stat_in.at[m, k], stat_send.at[h, t, k], stat_recv.at[h, t, k], (lax.rem(r + k, n_ra), c))

    def gather_plane(h, t, k):
        mine = rows_at(row_of(h, t) + core * half_rows + y * quarter, quarter)
        lands = stream.at[mine, pl.ds(0, width) if k == 1 else other_cols]
        send, recv = ((xg_send, xg_recv), (yg_send, yg_recv), (dg_send, dg_recv))[k]
        return remote(stream.at[mine, pl.ds(0, width)], lands, send.at[h, t], recv.at[h, t], (x_peer, y_peer, far_peer)[k])

    def gather_core(h, t, last):
        mine = rows_at(row_of(h, t) + core * half_rows, half_rows)
        cols = pl.ds(0, width) if last else pl.ds(0, 2 * width)
        return remote(stream.at[mine, cols], stream.at[mine, cols], cg_send.at[h, t], cg_recv.at[h, t], core_peer)

    def out_copy(h, t):
        at = pl.ds(row_of(h, t), rows)
        return pltpu.make_async_copy(stream.at[at, pl.ds(0, width)], out_hbm.at[at, :], out_sem.at[1 + h * nt + t])

    kept_half = pl.multiple_of(core * half_rows, half_rows)
    sent_half = pl.multiple_of((1 - core) * half_rows, half_rows)
    kept = pl.multiple_of(core * half_rows + y * quarter, quarter)
    sent = pl.multiple_of(core * half_rows + (1 - y) * quarter, quarter)

    def end_core(h, layer, t):
        m = h * nt + t
        core_out[m] = acc[m, pl.ds(sent_half, half_rows), :].astype(BF16)
        core_copy(h, t).start()

    def end_plane(h, layer, t):
        m = h * nt + t
        core_copy(h, t).wait()
        acc[m, pl.ds(kept_half, half_rows), :] += core_in[m].astype(F32)
        plane_out[m, 2] = acc[m, pl.ds(sent, quarter), pl.ds(width, width)].astype(BF16)
        plane_copy(h, t, 2).start()
        plane_out[m, 0] = acc[m, pl.ds(kept, quarter), pl.ds(width, width)].astype(BF16)
        plane_copy(h, t, 0).start()
        plane_out[m, 1] = acc[m, pl.ds(sent, quarter), pl.ds(0, width)].astype(BF16)
        plane_copy(h, t, 1).start()

    def lane_fold(v):
        total_v = v[:, :UNIT]
        for at in range(UNIT, width, UNIT):
            total_v = total_v + v[:, at:at + UNIT]
        return total_v

    def across(a, b):
        return lax.dot_general(a, b, (((1,), (1,)), ((), ())), preferred_element_type=F32, precision=lax.Precision.HIGHEST)

    def end_stats(h, layer, t):
        m = h * nt + t
        branch = acc[m, pl.ds(kept, quarter), pl.ds(0, width)]
        for k in range(3):
            plane_copy(h, t, k).wait()
            branch = branch + plane_in[m, k].astype(F32)
        mine = stream[rows_at(row_of(h, t) + kept, quarter), pl.ds(0, width)]
        mixed = RESIDUAL * mine.astype(F32) + branch
        acc[m, pl.ds(kept, quarter), pl.ds(0, width)] = mixed
        ones = jnp.ones((8, UNIT), F32)
        plain = across(ones, lane_fold(mixed))
        squared = across(ones, lane_fold(mixed * mixed))
        at = lax.broadcasted_iota(jnp.int32, plain.shape, 0)
        stat_out[m] = jnp.where(at < 4, plain, squared)
        for k in range(1, n_ra):
            stat_copy(h, t, k).start()

    def end_norm(h, layer, t):
        m = h * nt + t
        whole = stat_out[m]
        for k in range(1, n_ra):
            stat_copy(h, t, k).wait()
            whole = whole + stat_in[m, k]
        eye = (lax.broadcasted_iota(jnp.int32, (quarter, quarter), 0) == lax.broadcasted_iota(jnp.int32, (quarter, quarter), 1)).astype(F32)
        turned = across(eye, whole)
        mean = turned[:, 0:1] / full_width
        var = turned[:, 4:5] / full_width - mean * mean
        mixed = acc[m, pl.ds(kept, quarter), pl.ds(0, width)]
        normed = (mixed - mean) * lax.rsqrt(var + EPSILON)
        normed = normed * gain[pl.ds(layer, 1), :] + shift[pl.ds(layer, 1), :]
        stream[rows_at(row_of(h, t) + kept, quarter), pl.ds(0, width)] = normed.astype(BF16)

        @pl.when(layer < layers - 1)
        def _():
            gather_plane(h, t, 2).start()
            gather_plane(h, t, 0).start()

        gather_plane(h, t, 1).start()

    def end_gather_core(h, layer, t):
        @pl.when(layer < layers - 1)
        def _():
            for k in range(3):
                gather_plane(h, t, k).wait()
            gather_core(h, t, False).start()

        @pl.when(layer == layers - 1)
        def _():
            gather_plane(h, t, 1).wait()
            gather_core(h, t, True).start()

    def end_sent(h, layer, t):
        @pl.when(layer < layers - 1)
        def _():
            gather_core(h, t, False).wait_send()

        @pl.when(layer == layers - 1)
        def _():
            gather_core(h, t, True).wait()
            out_copy(h, t).start()

    longest = (HOP + BACK) * (groups - 1)

    def lag_sum(h):
        return HOP * place(h)[0]

    def lag_hid(h):
        return longest - BACK * place(h)[0]

    stages = (
        (lambda h: lag_hid(h), end_core),
        (lambda h: lag_hid(h) + ENDS[0], end_plane),
        (lambda h: lag_hid(h) + ENDS[1], end_stats),
        (lambda h: longest + ENDS[2], end_norm),
        (lambda h: longest + ENDS[3], end_gather_core),
        (lambda h: longest + ENDS[4], end_sent),
    )

    p0, p1 = place(0)[0], place(1)[0]
    p_low, p_high = jnp.minimum(p0, p1), jnp.maximum(p0, p1)

    first_layer = -(-(per_layer - AHEAD) // 3) * EARLY_OF

    def body(s, _):
        late = jnp.maximum(s - first_layer, 0)
        early = s < first_layer
        turn = jnp.where(early, lax.rem(s, EARLY_OF), lax.rem(late, LATE_OF))
        w = jnp.where(early, AHEAD + (s // EARLY_OF) * 3, per_layer + (late // LATE_OF) * 3) + turn
        most = jnp.where(early, per_layer, n_messages)

        @pl.when((turn < 3) & (w < most))
        def _():
            issued(w - IN_FLIGHT)
            issue(w)

        for step, act in zip(LATE, (pass_y, pass_core, passed)):
            @pl.when(s == step)
            def _(act=act):
                act(range(soon, nt))

        ok, layer_w, j_w = at_step(s, HOP * p_low)
        t_w, c_w = order(j_w)

        @pl.when(ok & (t_w == 0))
        def _():
            gu_copy(layer_w, c_w, 0).wait_recv()
            gu_copy(layer_w, c_w, 1).wait_recv()

        ok, layer_d, j_d = at_step(s, longest - BACK * p_high)
        t_d, c_d = order(j_d)

        @pl.when(ok & (t_d == 0))
        def _():
            d_copy(layer_d, c_d).wait_recv()

        for h in range(2):
            p, _, _ = place(h)
            ok, layer, j = at_step(s, lag_sum(h) + SENT)

            @pl.when(ok & (p < groups - 1))
            def _(h=h, layer=layer, j=j):
                sum_copy(h, layer, j).wait_send()

            ok, layer, j = at_step(s, lag_hid(h) + SENT)

            @pl.when(ok & (p > 0))
            def _(h=h, layer=layer, j=j):
                hid_copy(h, layer, j).wait_send()

            ok, layer, j = at_step(s, lag_hid(h))

            @pl.when(ok & (p < groups - 1))
            def _(h=h, layer=layer, j=j):
                stage_hid(h, layer, j)

        for h in range(2):
            p, _, _ = place(h)
            ok, layer, j = at_step(s, lag_sum(h))

            @pl.when(ok)
            def _(h=h, layer=layer, j=j):
                stage_sum(h, layer, j)

            @pl.when(ok & (p == groups - 1))
            def _(h=h, layer=layer, j=j):
                stage_hid(h, layer, j)

        for h in range(2):
            ok, layer, j = at_step(s, lag_hid(h))

            @pl.when(ok)
            def _(h=h, layer=layer, j=j):
                stage_down(h, layer, j)

        for lag, stage in stages:
            for h in range(2):
                ok, layer, j = at_step(s, lag(h))

                @pl.when(ok)
                def _(h=h, stage=stage, layer=layer, j=j):
                    t, cc = order(j)

                    @pl.when(cc == nc - 1)
                    def _():
                        stage(h, layer, t)

        return 0

    lax.fori_loop(0, layers * steps + longest + ENDS[4], body, 0)
    for w in range(n_messages - IN_FLIGHT, n_messages):
        issued(jnp.int32(w))
    for t in range(nt):
        for h in range(2):
            out_copy(h, t).wait()


ENDS = (1, 4, 6, 9, 10)


def layer_gap(groups, nc, nt):
    after = (HOP + BACK) * (groups - 1) + ENDS[3] + 1
    ends = [2 * nc - 2, 2 * nc - 1] + [t * nc + nc - 1 for t in range(2, nt)]
    starts = [0, 1] + [t * nc for t in range(2, nt)]
    gap = max([0] + [2 * (ends[t] - starts[t] - nc * nt) + after for t in range(nt)])
    return gap


def fits(ra, cb, tokens, width, columns):
    units = columns // PAIR
    return (
        ra % PAIR == 0 and ra >= 2 * PAIR and cb == 4 and units % UNIT == 0 and units // UNIT > AHEAD
        and width % UNIT == 0 and tokens % (2 * TOKEN_PARTS * 4 * 16) == 0
    )


def per_device_kernel(inputs, gate_weight, up_weight, down_weight, norm_gain, norm_shift):
    ra = lax.axis_size("ra")
    tokens, width = inputs.shape
    layers, _, columns = gate_weight.shape
    groups, units = ra // PAIR, columns // PAIR
    nc, nt = units // UNIT, TOKEN_PARTS
    rows = tokens // (2 * nt)
    slots, chunks = nc * nt, 2 * nt
    dma = pltpu.SemaphoreType.DMA
    scratch = [
        pltpu.VMEM((layers, nc, 2 * width, 2 * UNIT), BF16),
        pltpu.VMEM((layers, nc, UNIT, 2 * width), BF16),
        pltpu.VMEM((tokens, 2 * width), BF16),
        pltpu.VMEM((2, slots, rows, 2 * UNIT), BF16),
        pltpu.VMEM((2, slots, rows, UNIT), BF16),
        pltpu.VMEM((chunks, rows, 2 * width), F32),
        pltpu.VMEM((chunks, rows // 2, 2 * width), BF16),
        pltpu.VMEM((chunks, rows // 2, 2 * width), BF16),
        pltpu.VMEM((chunks, 3, rows // 4, width), BF16),
        pltpu.VMEM((chunks, 3, rows // 4, width), BF16),
        pltpu.VMEM((chunks, 8, rows // 4), F32),
        pltpu.VMEM((chunks, ra, 8, rows // 4), F32),
        dma((2, layers, nc, 2)),
        dma((layers, nc, 2)), dma((layers, nc, 2)), dma((layers, nc)), dma((layers, nc)),
        dma((2, 4)), dma((2, slots)), dma((2, 4)), dma((2, slots)),
        dma((2, nt)), dma((2, nt)), dma((2, nt, 3)), dma((2, nt, 3)),
        dma((2, nt, ra)), dma((2, nt, ra)),
        dma((2, nt)), dma((2, nt)), dma((2, nt)), dma((2, nt)), dma((2, nt)), dma((2, nt)), dma((2, nt)), dma((2, nt)),
        dma((1 + chunks,)),
    ]
    anywhere, near = pl.BlockSpec(memory_space=pl.ANY), pl.BlockSpec(memory_space=pltpu.VMEM)
    return pl.pallas_call(
        functools.partial(layer_kernel, groups),
        out_shape=jax.ShapeDtypeStruct((tokens, width), BF16),
        in_specs=[anywhere] * 4 + [near] * 2,
        out_specs=anywhere,
        scratch_shapes=scratch,
        compiler_params=pltpu.CompilerParams(has_side_effects=True, vmem_limit_bytes=62 * 2**20),
    )(inputs, gate_weight, up_weight, down_weight, norm_gain, norm_shift)


def per_device_any(inputs, gate_weight, up_weight, down_weight, norm_gain, norm_shift):
    ra, cb = lax.axis_size("ra"), lax.axis_size("cb")
    run = per_device_kernel if fits(ra, cb, *inputs.shape, gate_weight.shape[2]) else per_device
    return run(inputs, gate_weight, up_weight, down_weight, norm_gain, norm_shift)


def solution(mesh):
    return jax.shard_map(
        per_device_any,
        mesh=mesh,
        in_specs=(
            P(None, "ra"),
            P(None, "ra", "cb"),
            P(None, "ra", "cb"),
            P(None, "cb", "ra"),
            P(None, "ra"),
            P(None, "ra"),
        ),
        out_specs=P(None, "ra"),
        check_vma=False,
    )
```

```python
import functools

import jax
import jax.numpy as jnp
from jax import lax
from jax.experimental import pallas as pl
from jax.experimental.pallas import tpu as pltpu
from jax.sharding import PartitionSpec as P

LAYERS = 2
RESIDUAL = 0.5
EPSILON = 1e-05
PAIR = 2
TOKEN_CHUNKS = 3
COLUMN_CHUNKS = 2
BF16 = jnp.bfloat16
F32 = jnp.float32


def dot(a, b):
    return jnp.dot(a, b, preferred_element_type=F32)


def axis_ring(total, stride, size):
    perm = []
    for i in range(total):
        at = (i // stride) % size
        perm.append((i, i + (((at + 1) % size) - at) * stride))
    return perm


def xor_perm(total, bit):
    return [(i, i ^ bit) for i in range(total)]


def swap(x, axis):
    return lax.ppermute(x, axis, xor_perm(lax.axis_size(axis), 1))


def part(x, at, size, dim=0):
    return lax.dynamic_slice_in_dim(x, at * size, size, dim)


def ring_reduce(block, axis, stride, size, me):
    perm = axis_ring(lax.axis_size(axis), stride, size)
    total = block(lax.rem(me + size - 1, size))
    for step in range(1, size):
        arrived = lax.ppermute(total.astype(BF16), axis, perm)
        total = arrived.astype(F32) + block(lax.rem(me + 2 * size - 1 - step, size))
    return total


def ring_gather(x, axis, stride, size, me):
    perm = axis_ring(lax.axis_size(axis), stride, size)
    rows = x.shape[0]
    whole = jnp.zeros((rows * size,) + x.shape[1:], x.dtype)
    whole = lax.dynamic_update_slice_in_dim(whole, x, me * rows, 0)
    for step in range(1, size):
        x = lax.ppermute(x, axis, perm)
        owner = lax.rem(me + size - step, size)
        whole = lax.dynamic_update_slice_in_dim(whole, x, owner * rows, 0)
    return whole


def swap_gather(x, axis, me):
    other = swap(x, axis)
    first = jnp.where(me == 0, x, other)
    second = jnp.where(me == 0, other, x)
    return jnp.concatenate((first, second), axis=0)


def sum_over_ra(stats):
    total = lax.axis_size("ra")
    if total & (total - 1):
        return lax.psum(stats, "ra")
    bit = 1
    while bit < total:
        stats = stats + lax.ppermute(stats, "ra", xor_perm(total, bit))
        bit *= 2
    return stats


def cuts_of(width):
    step = -(-width // COLUMN_CHUNKS)
    step = min(width, -(-step // 128) * 128)
    return [(s, min(step, width - s)) for s in range(0, width, step)]


def per_device(inputs, gate_weight, up_weight, down_weight, norm_gain, norm_shift):
    ra, cb = lax.axis_size("ra"), lax.axis_size("cb")
    r, c = lax.axis_index("ra"), lax.axis_index("cb")
    groups, rows_y = ra // PAIR, cb // 2
    q, g = lax.rem(r, PAIR), r // PAIR
    core, y = lax.rem(c, 2), c // 2
    tokens, width = inputs.shape
    full_width = width * ra
    columns = gate_weight.shape[2]
    half = columns // PAIR
    cuts = cuts_of(half)
    chunk = tokens // TOKEN_CHUNKS

    queue = [None]

    def queued_swap(away):
        if queue[0] is not None:
            away, queue[0] = lax.optimization_barrier((away, queue[0]))
        queue[0] = swap(away, "ra")
        return queue[0]

    def weights_of(layer):
        kept, sent = q * half, (1 - q) * half
        pairs, downs = [], []
        for start, size in cuts:
            own = jnp.concatenate(
                [lax.dynamic_slice(w, (layer, 0, kept + start), (1, width, size))[0] for w in (gate_weight, up_weight)], axis=1
            )
            away = jnp.concatenate(
                [lax.dynamic_slice(w, (layer, 0, sent + start), (1, width, size))[0] for w in (gate_weight, up_weight)], axis=1
            )
            pairs.append((own, queued_swap(away)))
        for start, size in cuts:
            own = lax.dynamic_slice(down_weight, (layer, kept + start, 0), (1, size, width))[0]
            away = lax.dynamic_slice(down_weight, (layer, sent + start, 0), (1, size, width))[0]
            downs.append((own, queued_swap(away)))
        return pairs, downs

    streams = []
    for k in range(TOKEN_CHUNKS):
        own = inputs[k * chunk:(k + 1) * chunk]
        over = swap(part(own, core, chunk // 2), "ra")
        streams.append((own, swap_gather(over, "cb", core)))

    gate_open = None
    for layer in range(LAYERS):
        pairs, downs = weights_of(layer)
        last = layer == LAYERS - 1
        after = []
        for own, other in streams:
            block_rows = chunk // groups
            outs_own, outs_other = 0.0, 0.0
            if gate_open is not None:
                own, other, _ = lax.optimization_barrier((own, other, gate_open))
            opened = []
            for (w_own, w_other), (d_own, d_other) in zip(pairs, downs):
                size = d_own.shape[0]

                def block(at):
                    return dot(part(own, at, block_rows), w_own) + dot(part(other, at, block_rows), w_other)

                total = ring_reduce(block, "ra", PAIR, groups, g)
                hidden = (jax.nn.silu(total[:, :size]) * total[:, size:]).astype(BF16)
                opened.append(hidden)
                hidden = ring_gather(hidden, "ra", PAIR, groups, g)
                outs_own = outs_own + dot(hidden, d_own)
                outs_other = outs_other + dot(hidden, d_other)
            gate_open = tuple(h[:1] for h in opened)
            out = jnp.concatenate((outs_own, outs_other), axis=1)
            out = part(out, core, chunk // 2) + swap(part(out, 1 - core, chunk // 2).astype(BF16), "cb").astype(F32)
            rows = chunk // cb
            out = ring_reduce(lambda at: part(out, at, rows), "cb", 2, rows_y, y)
            branch = out[:, :width] + swap(out[:, width:].astype(BF16), "ra").astype(F32)
            mine = lax.dynamic_slice_in_dim(own, core * (chunk // 2) + y * rows, rows, 0)
            mixed = RESIDUAL * mine.astype(F32) + branch
            stats = sum_over_ra(jnp.stack((jnp.sum(mixed, axis=1), jnp.sum(mixed * mixed, axis=1))))
            mean = stats[0] / full_width
            var = stats[1] / full_width - mean * mean
            normed = (mixed - mean[:, None]) * lax.rsqrt(var + EPSILON)[:, None]
            normed = (normed * norm_gain[layer] + norm_shift[layer]).astype(BF16)
            if not last:
                normed = jnp.concatenate((normed, swap(normed, "ra")), axis=1)
            whole = swap_gather(ring_gather(normed, "cb", 2, rows_y, y), "cb", core)
            after.append(whole if last else (whole[:, :width], whole[:, width:]))
        streams = after
    return jnp.concatenate(streams, axis=0)


UNIT = 128
TOKEN_PARTS = 3
HOP = 3
BACK = 3
SENT = 4
LEAD = 5
AHEAD = 10
IN_FLIGHT = 8
EARLY_OF = 4
LATE_OF = 7
LATE = (6, 10, 14)
MESH_ID = pl.DeviceIdType.MESH


def layer_kernel(
    groups, x_hbm, gate_hbm, up_hbm, down_hbm, gain, shift, out_hbm,
    wgu, wd, stream, sums, hid, acc, core_out, core_in, plane_out, plane_in, stat_out, stat_in,
    own_sem, wgu_send, wgu_recv, wd_send, wd_recv, sum_send, sum_recv, hid_send, hid_recv,
    core_send, core_recv, plane_send, plane_recv, stat_send, stat_recv,
    xg_send, xg_recv, yg_send, yg_recv, dg_send, dg_recv, cg_send, cg_recv, out_sem,
):
    n_ra = 2 * groups
    tokens, width = x_hbm.shape
    full_width = width * n_ra
    layers, nc = wgu.shape[0], wgu.shape[1]
    nt = acc.shape[0] // 2
    rows = acc.shape[1]
    half_rows, quarter = rows // 2, rows // 4
    used = nc * nt
    steps = 2 * used + layer_gap(groups, nc, nt)
    units = nc * UNIT

    r, c = lax.axis_index("ra"), lax.axis_index("cb")
    q, g = lax.rem(r, 2), r // 2
    core, y = lax.rem(c, 2), c // 2
    x_peer = (r + 1 - 2 * q, c)
    y_peer = (r, (1 - y) * 2 + core)
    core_peer = (r, y * 2 + 1 - core)
    far_peer = (x_peer[0], y_peer[1])

    def place(h):
        p = (groups - 1 - g) if h == 0 else g
        ahead = (r - 2, c) if h == 0 else (r + 2, c)
        back = (r + 2, c) if h == 0 else (r - 2, c)
        return p, ahead, back

    def remote(src, dst, send, recv, to):
        return pltpu.make_async_remote_copy(src_ref=src, dst_ref=dst, send_sem=send, recv_sem=recv, device_id=to, device_id_type=MESH_ID)

    def order(j):
        both = j < 2 * nc
        return jnp.where(both, lax.rem(j, 2), j // nc), jnp.where(both, j // 2, lax.rem(j, nc))

    def at_step(s, lag):
        n = s - lag
        layer = jnp.maximum(n, 0) // steps
        j2 = n - layer * steps
        return (n >= 0) & (layer < layers) & (j2 < 2 * used) & (lax.rem(jnp.maximum(j2, 0), 2) == 0), layer, j2 // 2

    def row_of(h, t):
        return pl.multiple_of(h * (nt * rows) + t * rows, rows)

    def rows_at(start, size):
        return pl.ds(pl.multiple_of(start, quarter), size)

    def gu_copy(layer, cc, which):
        src = gate_hbm if which == 0 else up_hbm
        cols = pl.ds(pl.multiple_of((1 - q) * units + cc * UNIT, UNIT), UNIT)
        return remote(
            src.at[layer, :, cols],
            wgu.at[layer, cc, pl.ds(width, width), pl.ds(which * UNIT, UNIT)],
            wgu_send.at[layer, cc, which], wgu_recv.at[layer, cc, which], x_peer,
        )

    def d_copy(layer, cc):
        src_rows = pl.ds(pl.multiple_of((1 - q) * units + cc * UNIT, UNIT), UNIT)
        return remote(
            down_hbm.at[layer, src_rows, :],
            wd.at[layer, cc, :, pl.ds(width, width)],
            wd_send.at[layer, cc], wd_recv.at[layer, cc], x_peer,
        )

    per_layer = 3 * nc
    n_messages = layers * per_layer

    def message(w, act):
        layer = w // per_layer
        k = w - layer * per_layer
        k2 = k - 2 * LEAD
        k3 = k2 - 3 * (nc - LEAD)
        m = jnp.maximum(k2, 0) // 3
        turn = jnp.maximum(k2, 0) - 3 * m
        early = k2 < 0
        is_down = jnp.logical_not(early) & ((k3 >= 0) | (turn == 0))
        which = jnp.where(early, lax.rem(k, 2), turn - 1)
        gu_at = jnp.where(early, k // 2, LEAD + m)
        d_at = jnp.where(k3 >= 0, nc - LEAD + k3, m)

        @pl.when(is_down)
        def _():
            act(d_copy(layer, d_at))

        for part_at in range(2):
            @pl.when(jnp.logical_not(is_down) & (which == part_at))
            def _(part_at=part_at):
                act(gu_copy(layer, gu_at, part_at))

    def issue(w):
        message(w, lambda copy: copy.start())

    def issued(w):
        message(w, lambda copy: copy.wait_send())

    def own_gu(layer, cc, which):
        src = gate_hbm if which == 0 else up_hbm
        cols = pl.ds(pl.multiple_of(q * units + cc * UNIT, UNIT), UNIT)
        return pltpu.make_async_copy(
            src.at[layer, :, cols], wgu.at[layer, cc, pl.ds(0, width), pl.ds(which * UNIT, UNIT)], own_sem.at[0, layer, cc, which]
        )

    def own_d(layer, cc):
        src_rows = pl.ds(pl.multiple_of(q * units + cc * UNIT, UNIT), UNIT)
        return pltpu.make_async_copy(down_hbm.at[layer, src_rows, :], wd.at[layer, cc, :, pl.ds(0, width)], own_sem.at[1, layer, cc, 0])

    own_x = pltpu.make_async_copy(x_hbm, stream.at[:, pl.ds(0, width)], out_sem.at[0])

    other_cols = pl.ds(width, width)

    def first_x(h, t):
        mine = rows_at(row_of(h, t) + core * half_rows + y * quarter, quarter)
        return remote(x_hbm.at[mine, :], stream.at[mine, other_cols], xg_send.at[h, t], xg_recv.at[h, t], x_peer)

    def first_y(h, t):
        mine = rows_at(row_of(h, t) + core * half_rows + y * quarter, quarter)
        view = stream.at[mine, other_cols]
        return remote(view, view, yg_send.at[h, t], yg_recv.at[h, t], y_peer)

    def first_core(h, t):
        mine = rows_at(row_of(h, t) + core * half_rows, half_rows)
        view = stream.at[mine, other_cols]
        return remote(view, view, cg_send.at[h, t], cg_recv.at[h, t], core_peer)

    soon = min(2, nt)
    for t in range(soon):
        for h in range(2):
            first_x(h, t).start()
    own_x.start()
    for w in range(AHEAD):
        issue(jnp.int32(w))
        if w == 1:
            for t in range(soon, nt):
                for h in range(2):
                    first_x(h, t).start()

    def pass_y(chunks):
        for t in chunks:
            for h in range(2):
                first_x(h, t).wait_recv()
                first_y(h, t).start()

    def pass_core(chunks):
        for t in chunks:
            for h in range(2):
                first_y(h, t).wait_recv()
                first_core(h, t).start()

    def passed(chunks):
        for t in chunks:
            for h in range(2):
                first_x(h, t).wait_send()
                first_y(h, t).wait_send()
                first_core(h, t).wait_send()

    def own_start(j, _):
        layer, cc = j // nc, lax.rem(j, nc)
        own_gu(layer, cc, 0).start()
        own_gu(layer, cc, 1).start()
        own_d(layer, cc).start()
        return 0

    def own_wait(j, _):
        layer, cc = j // nc, lax.rem(j, nc)
        own_gu(layer, cc, 0).wait()
        own_gu(layer, cc, 1).wait()
        own_d(layer, cc).wait()
        return 0

    lax.fori_loop(0, layers * nc, own_start, 0)
    pass_y(range(soon))
    own_x.wait()
    pass_core(range(soon))
    lax.fori_loop(0, layers * nc, own_wait, 0)
    passed(range(soon))
    for w in range(AHEAD - IN_FLIGHT):
        issued(jnp.int32(w))

    def sum_copy(h, layer, j):
        t, cc = order(j)
        _, ahead, _ = place(h)
        view = sums.at[h, t * nc + cc]
        return remote(view, view, sum_send.at[h, lax.rem(layer * used + j, 4)], sum_recv.at[h, t * nc + cc], ahead)

    def hid_copy(h, layer, j):
        t, cc = order(j)
        _, _, back = place(h)
        view = hid.at[h, t * nc + cc]
        return remote(view, view, hid_send.at[h, lax.rem(layer * used + j, 4)], hid_recv.at[h, t * nc + cc], back)

    def stage_sum(h, layer, j):
        p, _, _ = place(h)
        t, cc = order(j)

        @pl.when((cc == 0) & (layer == 0))
        def _():
            first_core(h, t).wait_recv()

        @pl.when((cc == 0) & (layer > 0))
        def _():
            gather_core(h, t, False).wait_recv()

        slot = t * nc + cc
        own = jnp.dot(stream[pl.ds(row_of(h, t), rows), :], wgu[layer, cc], preferred_element_type=F32)

        @pl.when(p == 0)
        def _():
            sums[h, slot] = own.astype(BF16)

        @pl.when((p > 0) & (p < groups - 1))
        def _():
            sum_copy(h, layer, j).wait_recv()
            sums[h, slot] = (sums[h, slot].astype(F32) + own).astype(BF16)

        @pl.when(p < groups - 1)
        def _():
            sum_copy(h, layer, j).start()

        @pl.when(p == groups - 1)
        def _():
            sum_copy(h, layer, j).wait_recv()
            whole = sums[h, slot].astype(F32) + own
            hid[h, slot] = (jax.nn.silu(whole[:, :UNIT]) * whole[:, UNIT:]).astype(BF16)

    def stage_hid(h, layer, j):
        p, _, _ = place(h)

        @pl.when(p < groups - 1)
        def _():
            hid_copy(h, layer, j).wait_recv()

        @pl.when(p > 0)
        def _():
            hid_copy(h, layer, j).start()

    def stage_down(h, layer, j):
        t, cc = order(j)
        part_sum = jnp.dot(hid[h, t * nc + cc], wd[layer, cc], preferred_element_type=F32)
        m = h * nt + t

        @pl.when(cc == 0)
        def _():
            acc[m] = part_sum

        @pl.when(cc > 0)
        def _():
            acc[m] += part_sum

    def core_copy(h, t):
        m = h * nt + t
        return remote(core_out.at[m], core_in.at[m], core_send.at[h, t], core_recv.at[h, t], core_peer)

    def plane_copy(h, t, k):
        m = h * nt + t
        return remote(
            plane_out.at[m, k], plane_in.at[m, k], plane_send.at[h, t, k], plane_recv.at[h, t, k], (x_peer, y_peer, far_peer)[k]
        )

    def stat_copy(h, t, k):
        m = h * nt + t
        return remote(stat_out.at[m], stat_in.at[m, k], stat_send.at[h, t, k], stat_recv.at[h, t, k], (lax.rem(r + k, n_ra), c))

    def gather_plane(h, t, k):
        mine = rows_at(row_of(h, t) + core * half_rows + y * quarter, quarter)
        lands = stream.at[mine, pl.ds(0, width) if k == 1 else other_cols]
        send, recv = ((xg_send, xg_recv), (yg_send, yg_recv), (dg_send, dg_recv))[k]
        return remote(stream.at[mine, pl.ds(0, width)], lands, send.at[h, t], recv.at[h, t], (x_peer, y_peer, far_peer)[k])

    def gather_core(h, t, last):
        mine = rows_at(row_of(h, t) + core * half_rows, half_rows)
        cols = pl.ds(0, width) if last else pl.ds(0, 2 * width)
        return remote(stream.at[mine, cols], stream.at[mine, cols], cg_send.at[h, t], cg_recv.at[h, t], core_peer)

    def out_copy(h, t):
        at = pl.ds(row_of(h, t), rows)
        return pltpu.make_async_copy(stream.at[at, pl.ds(0, width)], out_hbm.at[at, :], out_sem.at[1 + h * nt + t])

    kept_half = pl.multiple_of(core * half_rows, half_rows)
    sent_half = pl.multiple_of((1 - core) * half_rows, half_rows)
    kept = pl.multiple_of(core * half_rows + y * quarter, quarter)
    sent = pl.multiple_of(core * half_rows + (1 - y) * quarter, quarter)

    def end_core(h, layer, t):
        m = h * nt + t
        core_out[m] = acc[m, pl.ds(sent_half, half_rows), :].astype(BF16)
        core_copy(h, t).start()

    def end_plane(h, layer, t):
        m = h * nt + t
        core_copy(h, t).wait()
        acc[m, pl.ds(kept_half, half_rows), :] += core_in[m].astype(F32)
        plane_out[m, 2] = acc[m, pl.ds(sent, quarter), pl.ds(width, width)].astype(BF16)
        plane_copy(h, t, 2).start()
        plane_out[m, 0] = acc[m, pl.ds(kept, quarter), pl.ds(width, width)].astype(BF16)
        plane_copy(h, t, 0).start()
        plane_out[m, 1] = acc[m, pl.ds(sent, quarter), pl.ds(0, width)].astype(BF16)
        plane_copy(h, t, 1).start()

    def lane_fold(v):
        total_v = v[:, :UNIT]
        for at in range(UNIT, width, UNIT):
            total_v = total_v + v[:, at:at + UNIT]
        return total_v

    def across(a, b):
        return lax.dot_general(a, b, (((1,), (1,)), ((), ())), preferred_element_type=F32, precision=lax.Precision.HIGHEST)

    def end_stats(h, layer, t):
        m = h * nt + t
        branch = acc[m, pl.ds(kept, quarter), pl.ds(0, width)]
        for k in range(3):
            plane_copy(h, t, k).wait()
            branch = branch + plane_in[m, k].astype(F32)
        mine = stream[rows_at(row_of(h, t) + kept, quarter), pl.ds(0, width)]
        mixed = RESIDUAL * mine.astype(F32) + branch
        acc[m, pl.ds(kept, quarter), pl.ds(0, width)] = mixed
        ones = jnp.ones((8, UNIT), F32)
        plain = across(ones, lane_fold(mixed))
        squared = across(ones, lane_fold(mixed * mixed))
        at = lax.broadcasted_iota(jnp.int32, plain.shape, 0)
        stat_out[m] = jnp.where(at < 4, plain, squared)
        for k in range(1, n_ra):
            stat_copy(h, t, k).start()

    def end_norm(h, layer, t):
        m = h * nt + t
        whole = stat_out[m]
        for k in range(1, n_ra):
            stat_copy(h, t, k).wait()
            whole = whole + stat_in[m, k]
        eye = (lax.broadcasted_iota(jnp.int32, (quarter, quarter), 0) == lax.broadcasted_iota(jnp.int32, (quarter, quarter), 1)).astype(F32)
        turned = across(eye, whole)
        mean = turned[:, 0:1] / full_width
        var = turned[:, 4:5] / full_width - mean * mean
        mixed = acc[m, pl.ds(kept, quarter), pl.ds(0, width)]
        normed = (mixed - mean) * lax.rsqrt(var + EPSILON)
        normed = normed * gain[pl.ds(layer, 1), :] + shift[pl.ds(layer, 1), :]
        stream[rows_at(row_of(h, t) + kept, quarter), pl.ds(0, width)] = normed.astype(BF16)

        @pl.when(layer < layers - 1)
        def _():
            gather_plane(h, t, 2).start()
            gather_plane(h, t, 0).start()

        gather_plane(h, t, 1).start()

    def end_gather_core(h, layer, t):
        @pl.when(layer < layers - 1)
        def _():
            for k in range(3):
                gather_plane(h, t, k).wait()
            gather_core(h, t, False).start()

        @pl.when(layer == layers - 1)
        def _():
            gather_plane(h, t, 1).wait()
            gather_core(h, t, True).start()

    def end_sent(h, layer, t):
        @pl.when(layer < layers - 1)
        def _():
            gather_core(h, t, False).wait_send()

        @pl.when(layer == layers - 1)
        def _():
            gather_core(h, t, True).wait()
            out_copy(h, t).start()

    longest = (HOP + BACK) * (groups - 1)

    def lag_sum(h):
        return HOP * place(h)[0]

    def lag_hid(h):
        return longest - BACK * place(h)[0]

    stages = (
        (lambda h: lag_hid(h), end_core),
        (lambda h: lag_hid(h) + ENDS[0], end_plane),
        (lambda h: lag_hid(h) + ENDS[1], end_stats),
        (lambda h: longest + ENDS[2], end_norm),
        (lambda h: longest + ENDS[3], end_gather_core),
        (lambda h: longest + ENDS[4], end_sent),
    )

    p0, p1 = place(0)[0], place(1)[0]
    p_low, p_high = jnp.minimum(p0, p1), jnp.maximum(p0, p1)

    first_layer = -(-(per_layer - AHEAD) // 3) * EARLY_OF

    def body(s, _):
        late = jnp.maximum(s - first_layer, 0)
        early = s < first_layer
        turn = jnp.where(early, lax.rem(s, EARLY_OF), lax.rem(late, LATE_OF))
        w = jnp.where(early, AHEAD + (s // EARLY_OF) * 3, per_layer + (late // LATE_OF) * 3) + turn
        most = jnp.where(early, per_layer, n_messages)

        @pl.when((turn < 3) & (w < most))
        def _():
            issued(w - IN_FLIGHT)
            issue(w)

        for step, act in zip(LATE, (pass_y, pass_core, passed)):
            @pl.when(s == step)
            def _(act=act):
                act(range(soon, nt))

        ok, layer_w, j_w = at_step(s, HOP * p_low)
        t_w, c_w = order(j_w)

        @pl.when(ok & (t_w == 0))
        def _():
            gu_copy(layer_w, c_w, 0).wait_recv()
            gu_copy(layer_w, c_w, 1).wait_recv()

        ok, layer_d, j_d = at_step(s, longest - BACK * p_high)
        t_d, c_d = order(j_d)

        @pl.when(ok & (t_d == 0))
        def _():
            d_copy(layer_d, c_d).wait_recv()

        for h in range(2):
            p, _, _ = place(h)
            ok, layer, j = at_step(s, lag_sum(h) + SENT)

            @pl.when(ok & (p < groups - 1))
            def _(h=h, layer=layer, j=j):
                sum_copy(h, layer, j).wait_send()

            ok, layer, j = at_step(s, lag_hid(h) + SENT)

            @pl.when(ok & (p > 0))
            def _(h=h, layer=layer, j=j):
                hid_copy(h, layer, j).wait_send()

            ok, layer, j = at_step(s, lag_hid(h))

            @pl.when(ok & (p < groups - 1))
            def _(h=h, layer=layer, j=j):
                stage_hid(h, layer, j)

        for h in range(2):
            p, _, _ = place(h)
            ok, layer, j = at_step(s, lag_sum(h))

            @pl.when(ok)
            def _(h=h, layer=layer, j=j):
                stage_sum(h, layer, j)

            @pl.when(ok & (p == groups - 1))
            def _(h=h, layer=layer, j=j):
                stage_hid(h, layer, j)

        for h in range(2):
            ok, layer, j = at_step(s, lag_hid(h))

            @pl.when(ok)
            def _(h=h, layer=layer, j=j):
                stage_down(h, layer, j)

        for lag, stage in stages:
            for h in range(2):
                ok, layer, j = at_step(s, lag(h))

                @pl.when(ok)
                def _(h=h, stage=stage, layer=layer, j=j):
                    t, cc = order(j)

                    @pl.when(cc == nc - 1)
                    def _():
                        stage(h, layer, t)

        return 0

    lax.fori_loop(0, layers * steps + longest + ENDS[4], body, 0)
    for w in range(n_messages - IN_FLIGHT, n_messages):
        issued(jnp.int32(w))
    for t in range(nt):
        for h in range(2):
            out_copy(h, t).wait()


ENDS = (1, 4, 6, 9, 10)


def layer_gap(groups, nc, nt):
    after = (HOP + BACK) * (groups - 1) + ENDS[3] + 1
    ends = [2 * nc - 2, 2 * nc - 1] + [t * nc + nc - 1 for t in range(2, nt)]
    starts = [0, 1] + [t * nc for t in range(2, nt)]
    gap = max([0] + [2 * (ends[t] - starts[t] - nc * nt) + after for t in range(nt)])
    return gap


def fits(ra, cb, tokens, width, columns):
    units = columns // PAIR
    return (
        ra % PAIR == 0 and ra >= 2 * PAIR and cb == 4 and units % UNIT == 0 and units // UNIT > AHEAD
        and width % UNIT == 0 and tokens % (2 * TOKEN_PARTS * 4 * 16) == 0
    )


def per_device_kernel(inputs, gate_weight, up_weight, down_weight, norm_gain, norm_shift):
    ra = lax.axis_size("ra")
    tokens, width = inputs.shape
    layers, _, columns = gate_weight.shape
    groups, units = ra // PAIR, columns // PAIR
    nc, nt = units // UNIT, TOKEN_PARTS
    rows = tokens // (2 * nt)
    slots, chunks = nc * nt, 2 * nt
    dma = pltpu.SemaphoreType.DMA
    scratch = [
        pltpu.VMEM((layers, nc, 2 * width, 2 * UNIT), BF16),
        pltpu.VMEM((layers, nc, UNIT, 2 * width), BF16),
        pltpu.VMEM((tokens, 2 * width), BF16),
        pltpu.VMEM((2, slots, rows, 2 * UNIT), BF16),
        pltpu.VMEM((2, slots, rows, UNIT), BF16),
        pltpu.VMEM((chunks, rows, 2 * width), F32),
        pltpu.VMEM((chunks, rows // 2, 2 * width), BF16),
        pltpu.VMEM((chunks, rows // 2, 2 * width), BF16),
        pltpu.VMEM((chunks, 3, rows // 4, width), BF16),
        pltpu.VMEM((chunks, 3, rows // 4, width), BF16),
        pltpu.VMEM((chunks, 8, rows // 4), F32),
        pltpu.VMEM((chunks, ra, 8, rows // 4), F32),
        dma((2, layers, nc, 2)),
        dma((layers, nc, 2)), dma((layers, nc, 2)), dma((layers, nc)), dma((layers, nc)),
        dma((2, 4)), dma((2, slots)), dma((2, 4)), dma((2, slots)),
        dma((2, nt)), dma((2, nt)), dma((2, nt, 3)), dma((2, nt, 3)),
        dma((2, nt, ra)), dma((2, nt, ra)),
        dma((2, nt)), dma((2, nt)), dma((2, nt)), dma((2, nt)), dma((2, nt)), dma((2, nt)), dma((2, nt)), dma((2, nt)),
        dma((1 + chunks,)),
    ]
    anywhere, near = pl.BlockSpec(memory_space=pl.ANY), pl.BlockSpec(memory_space=pltpu.VMEM)
    return pl.pallas_call(
        functools.partial(layer_kernel, groups),
        out_shape=jax.ShapeDtypeStruct((tokens, width), BF16),
        in_specs=[anywhere] * 4 + [near] * 2,
        out_specs=anywhere,
        scratch_shapes=scratch,
        compiler_params=pltpu.CompilerParams(has_side_effects=True, vmem_limit_bytes=62 * 2**20),
    )(inputs, gate_weight, up_weight, down_weight, norm_gain, norm_shift)


def per_device_any(inputs, gate_weight, up_weight, down_weight, norm_gain, norm_shift):
    ra, cb = lax.axis_size("ra"), lax.axis_size("cb")
    run = per_device_kernel if fits(ra, cb, *inputs.shape, gate_weight.shape[2]) else per_device
    return run(inputs, gate_weight, up_weight, down_weight, norm_gain, norm_shift)


def solution(mesh):
    return jax.shard_map(
        per_device_any,
        mesh=mesh,
        in_specs=(
            P(None, "ra"),
            P(None, "ra", "cb"),
            P(None, "ra", "cb"),
            P(None, "cb", "ra"),
            P(None, "ra"),
            P(None, "ra"),
        ),
        out_specs=P(None, "ra"),
        check_vma=False,
    )
```
